32 devices in a mesh: rep: 4 (over z), fs: 4 (over y, x), tp: 2 (over core).
Axes of the slice: x: 2, y: 2, z: 4, core: 2. Of those that a mesh axis runs over, the one named last changes fastest.
Arguments:
- tokens: bfloat16 [8192, 2048], P(('rep', 'fs')), may hold values from -6 to 6
- mix_gain: float32 [2048], replicated, may hold values from 0.1 to 1.9
- w_gate_b: bfloat16 [2048, 1024], P('fs', 'tp'), may hold values from -0.125 to 0.125
- w_gate_c: bfloat16 [2048, 1024], P('fs', 'tp'), may hold values from -0.125 to 0.125
- w_conv_in: bfloat16 [2048, 1024], P('fs', 'tp'), may hold values from -0.125 to 0.125
- conv_taps: float32 [3, 1024], P(None, 'tp'), may hold values from -3 to 3
- w_mix_out: bfloat16 [1024, 2048], P('tp', 'fs'), may hold values from -0.1875 to 0.1875
- ffn_gain: float32 [2048], replicated, may hold values from 0.1 to 1.9
- w_ffn_gate: bfloat16 [2048, 2816], P('fs', 'tp'), may hold values from -0.125 to 0.125
- w_ffn_up: bfloat16 [2048, 2816], P('fs', 'tp'), may hold values from -0.125 to 0.125
- w_ffn_down: bfloat16 [2816, 2048], P('tp', 'fs'), may hold values from -0.109375 to 0.109375
Outputs:
- layer_out: bfloat16 [8192, 2048], P(('rep', 'fs', 'tp'))
The draws below stay inside these ranges and needn't reach their ends.
All inputs are finite; a program needn't handle non-finite values.
Results may differ from the reference program's by a relative error of at most 0.014.
Values may be sent and summed in bfloat16 or wider, within the bound.
A program may use at most 64 MiB of HBM per device.

```python
import jax
import jax.numpy as jnp
from jax import lax

D = 2048
DC = 1024
FF = 2816
LEN = 128
TOKENS = 8192
N_TP = 2


def shard_levels(own_key, shape, pieces, smallest, top_value):
    loudness = 1.0
    for dim, parts in pieces:
        draws = jax.random.uniform(jax.random.fold_in(jax.random.fold_in(own_key, 6), dim), (parts,), jnp.float32, smallest / len(pieces), top_value / len(pieces))
        loudness = loudness * jnp.repeat(jnp.exp(draws), shape[dim] // parts).reshape((-1,) + (1,) * (len(shape) - 1 - dim))
    return loudness


def gaussian(rng, shape, scale, limit, cuts=(), held_as=jnp.bfloat16):
    loudness = shard_levels(rng, shape, cuts, -0.22, 0.18) if cuts else 1.0
    values = jax.random.normal(rng, shape, jnp.float32) * scale * loudness
    return jnp.minimum(jnp.maximum(values, -limit), limit).astype(held_as)


def setup_inputs(seed: int = 0) -> dict:
    keys = jax.random.split(jax.random.key(seed), 12)
    tokens = gaussian(keys[0], (TOKENS, D), 1.0, 6.0, ((0, 16),))
    mix_gain = jnp.clip(1.0 + 0.18 * jax.random.normal(keys[1], (D,), jnp.float32), 0.1, 1.9)
    w_gate_b = gaussian(keys[2], (D, DC), D ** -0.5, 0.125, ((0, 4), (1, 2)))
    w_gate_c = gaussian(keys[3], (D, DC), D ** -0.5, 0.125, ((0, 4), (1, 2)))
    w_conv_in = gaussian(keys[4], (D, DC), D ** -0.5, 0.125, ((0, 4), (1, 2)))
    conv_taps = gaussian(keys[5], (3, DC), 0.6, 3.0, ((1, 2),), jnp.float32)
    w_mix_out = gaussian(keys[6], (DC, D), DC ** -0.5, 0.1875, ((0, 2), (1, 4)))
    ffn_gain = jnp.clip(1.0 + 0.18 * jax.random.normal(keys[7], (D,), jnp.float32), 0.1, 1.9)
    w_ffn_gate = gaussian(keys[8], (D, FF), D ** -0.5, 0.125, ((0, 4), (1, 2)))
    w_ffn_up = gaussian(keys[9], (D, FF), D ** -0.5, 0.125, ((0, 4), (1, 2)))
    w_ffn_down = gaussian(keys[10], (FF, D), FF ** -0.5, 0.109375, ((0, 2), (1, 4)))
    return {"tokens": tokens, "mix_gain": mix_gain, "w_gate_b": w_gate_b, "w_gate_c": w_gate_c, "w_conv_in": w_conv_in, "conv_taps": conv_taps, "w_mix_out": w_mix_out, "ffn_gain": ffn_gain, "w_ffn_gate": w_ffn_gate, "w_ffn_up": w_ffn_up, "w_ffn_down": w_ffn_down}


EPSILON = 1e-06

def rms_scale(values, gain):
    return values * lax.rsqrt(lax.optimization_barrier(jnp.mean(values * values, axis=-1, keepdims=True)) + EPSILON) * gain

def causal_mix(product_in, conv_taps):
    shaped = product_in.reshape(product_in.shape[0] // LEN, LEN, product_in.shape[1])
    padded = jnp.pad(shaped, ((0, 0), (2, 0), (0, 0)))
    convolved = conv_taps[0] * padded[:, :-2] + conv_taps[1] * padded[:, 1:-1] + conv_taps[2] * padded[:, 2:]
    return convolved.reshape(product_in.shape)

def block_sum(acts, weight, blocks):
    block_width = acts.shape[1] // blocks

    def step(running, block_index):
        first = (block_index * block_width).astype(jnp.int32)
        partial_value = jnp.dot(lax.dynamic_slice_in_dim(acts, first, block_width, 1), lax.dynamic_slice_in_dim(weight, first, block_width, 0), preferred_element_type=jnp.float32)
        rounded = lax.optimization_barrier(partial_value.astype(jnp.bfloat16)).astype(jnp.float32)
        return (running + rounded, None)
    start_acc = jnp.zeros((acts.shape[0], weight.shape[1]), jnp.float32)
    running, _ = lax.scan(step, start_acc, jnp.arange(blocks, dtype=jnp.int32))
    return running

def reference(tokens, mix_gain, w_gate_b, w_gate_c, w_conv_in, conv_taps, w_mix_out, ffn_gain, w_ffn_gate, w_ffn_up, w_ffn_down):
    inputs = tokens.astype(jnp.float32)
    normed = rms_scale(inputs, mix_gain).astype(jnp.bfloat16)
    gate_b = jnp.dot(normed, w_gate_b, preferred_element_type=jnp.float32)
    gate_c = jnp.dot(normed, w_gate_c, preferred_element_type=jnp.float32)
    conv_in = jnp.dot(normed, w_conv_in, preferred_element_type=jnp.float32)
    convolved = causal_mix(gate_c * conv_in, conv_taps)
    gated = (gate_b * convolved).astype(jnp.bfloat16)
    stream = inputs + block_sum(gated, w_mix_out, N_TP)
    normed_two = rms_scale(stream, ffn_gain).astype(jnp.bfloat16)
    gate_part = jnp.dot(normed_two, w_ffn_gate, preferred_element_type=jnp.float32)
    up_part = jnp.dot(normed_two, w_ffn_up, preferred_element_type=jnp.float32)
    hidden = (jax.nn.silu(gate_part) * up_part).astype(jnp.bfloat16)
    return (stream + block_sum(hidden, w_ffn_down, N_TP)).astype(jnp.bfloat16)
```

```python
import functools

import jax
import jax.numpy as jnp
from jax import lax
from jax.experimental import pallas as pl
from jax.experimental.pallas import tpu as pltpu
from jax.sharding import PartitionSpec as P

LEN = 128
LANES = 128
EPSILON = 1e-06
MESH = pl.DeviceIdType.MESH
F32 = jnp.float32
BF16 = jnp.bfloat16


def rms_scale(values, gain):
    return values * lax.rsqrt(jnp.mean(values * values, axis=-1, keepdims=True) + EPSILON) * gain


def layer_kernel(
    tokens, wb, wc, wi, wm_in, wgu_in, wd_in, mix_gain, taps, ffn_gain,
    out,
    tok, normed, n2, WA, WM, WG, WD, gated, MP, RS, CB, RZ, hidden, OS, OW, RO, ZC, RF,
    load_sem, ds, dr, fs_, fr, tz, ts, sib_s, sib_r, z_s, z_r, n_s, n_r, o_s, o_r, q_s, q_r,
):
    n_fs, rows_d, _ = WA.shape
    ch = gated.shape[1]
    hid = hidden.shape[1]
    chip_rows = tokens.shape[0]
    blk = chip_rows // 2
    width = tokens.shape[1]
    cols = WM.shape[2]

    r = lax.axis_index("rep")
    f = lax.axis_index("fs")
    t = lax.axis_index("tp")
    p = lax.rem(r, 2)
    z_dev = {"rep": r + 1 - 2 * p}
    x_of = f + 1 - 2 * lax.rem(f, 2)
    y_of = lax.rem(f + 2, 4)
    d_of = lax.rem(x_of + 2, 4)
    x_dev, y_dev, s_dev = {"fs": x_of}, {"fs": y_of}, {"tp": 1 - t}

    def row_block(j, core):
        return pl.ds(pl.multiple_of(j * chip_rows + core * blk, blk), blk)

    chan = pl.ds(pl.multiple_of(p * ch, ch), ch)
    loads = []

    def load(src, dst):
        c = pltpu.make_async_copy(src, dst, load_sem.at[len(loads)])
        c.start()
        loads.append(c)
        return c

    l_wa = [load(w.at[:, chan], WA.at[f, :, pl.ds(i * ch, ch)]) for i, w in enumerate((wb, wc, wi))]
    l_tok = load(tokens, tok.at[pl.ds(pl.multiple_of(p * chip_rows, chip_rows), chip_rows)])
    l_wm = load(wm_in.at[chan, :], WM.at[f])
    l_wg = load(wgu_in, WG.at[f])
    l_wd = load(wd_in.at[pl.ds(pl.multiple_of(p * hid, 16), hid), :], WD.at[f])

    barrier = pltpu.get_barrier_semaphore()
    for dev in (x_dev, y_dev, z_dev, s_dev):
        pl.semaphore_signal(barrier, inc=1, device_id=dev, device_id_type=MESH)
    pl.semaphore_wait(barrier, 4)

    def remote(src, dst, s, rcv, dev):
        return pltpu.make_async_remote_copy(
            src_ref=src, dst_ref=dst, send_sem=s, recv_sem=rcv, device_id=dev, device_id_type=MESH
        )

    pieces = []
    for buf, parts in ((WA, 2), (WM, 1), (WG, 4), (WD, 2)):
        n = buf.shape[1] // parts
        pieces += [(buf, i * n, n) for i in range(parts)]

    def direct(k):
        buf, r0, n = pieces[k]
        ref = buf.at[f, pl.ds(r0, n)]
        return [remote(ref, ref, ds.at[k, c], dr.at[k, c], dev) for c, dev in ((0, x_dev), (1, y_dev))]

    def forward(k):
        buf, r0, n = pieces[k]
        a = buf.at[x_of, pl.ds(r0, n // 2)]
        b = buf.at[y_of, pl.ds(r0 + n // 2, n // 2)]
        return [
            remote(b, b, fs_.at[k, 0], fr.at[k, 0], x_dev),
            remote(a, a, fs_.at[k, 1], fr.at[k, 1], y_dev),
        ]

    sent = []

    def start(copies):
        for c in copies:
            c.start()
            sent.append(c)
        return copies

    D, F = {}, {}

    def send(k):
        D[k] = start(direct(k))

    def step(k, *more):
        for c in D[k]:
            c.wait_recv()
        F[k] = start(forward(k))
        for m in more:
            send(m)

    def arrived(*ks):
        for k in ks:
            for c in F[k]:
                c.wait_recv()

    for c in l_wa:
        c.wait()
    send(0)
    send(1)
    l_tok.wait()
    own = tok.at[row_block(p, t)]
    tz_copy = start([remote(own, own, tz.at[0], tz.at[1], z_dev)])[0]

    def norm_rows(base):
        def body(i, _):
            rows = pl.ds(pl.multiple_of(base + i * 64, 64), 64)
            normed[rows, :] = rms_scale(tok[rows, :].astype(F32), mix_gain[...]).astype(BF16)
            return 0

        lax.fori_loop(0, chip_rows // 64, body, 0)

    norm_rows(p * chip_rows)
    l_wm.wait()
    l_wg.wait()
    l_wd.wait()
    step(0, 2)
    step(1)
    tz_copy.wait_recv()
    got = tok.at[row_block(1 - p, t)]
    ts_copy = start([remote(got, got, ts.at[0], ts.at[1], s_dev)])[0]
    step(2, 3, 4)
    ts_copy.wait_recv()
    norm_rows((1 - p) * chip_rows)
    arrived(0, 1)

    tap = [taps[pl.ds(i, 1), chan] for i in range(3)]
    pos = lax.rem(lax.broadcasted_iota(jnp.int32, (blk, ch), 0), LEN)

    def mix_body(i, _):
        rows = pl.ds(pl.multiple_of(i * blk, blk), blk)
        x = normed[rows, :]

        def proj(q):
            w = WA[:, :, q * ch:(q + 1) * ch].reshape(width, ch)
            return jnp.dot(x, w, preferred_element_type=F32)

        pr = proj(1) * proj(2)
        one = jnp.where(pos >= 1, pltpu.roll(pr, 1, 0), 0.0)
        two = jnp.where(pos >= 2, pltpu.roll(pr, 2, 0), 0.0)
        conv = tap[0] * two + tap[1] * one + tap[2] * pr
        gated[rows, :] = (proj(0) * conv).astype(BF16)
        return 0

    lax.fori_loop(0, 2 * chip_rows // blk, mix_body, 0)
    arrived(2)

    def mix_out(j, core):
        rows = row_block(j, core)
        g = gated[rows, :]
        for s in range(n_fs):
            MP[rows, s * cols:(s + 1) * cols] = jnp.dot(
                g, WM[s], preferred_element_type=F32
            ).astype(BF16)

    sib = []
    for j in range(2):
        mix_out(j, 1 - t)
        sib += start([remote(MP.at[row_block(j, 1 - t)], RS.at[j], sib_s.at[j], sib_r.at[j], s_dev)])
    zc = []
    for j in range(2):
        mix_out(j, t)
        sib[j].wait_recv()

        def add_body(i, _, j=j):
            rows = pl.ds(pl.multiple_of(i * 64, 64), 64)
            mine = pl.ds(pl.multiple_of(j * chip_rows + t * blk + i * 64, 64), 64)
            CB[j, rows, :] = (MP[mine, :].astype(F32) + RS[j, rows, :].astype(F32)).astype(BF16)
            return 0

        lax.fori_loop(0, blk // 64, add_body, 0)
        zc += start([remote(CB.at[j], RZ.at[j], z_s.at[j], z_r.at[j], z_dev)])

    step(3, 5)
    step(4, 6)
    step(5, 7)
    nb = []

    def stream_block(j):
        zc[j].wait_recv()

        def body(i, _):
            rows = pl.ds(pl.multiple_of(i * 64, 64), 64)
            mine = pl.ds(pl.multiple_of(j * chip_rows + t * blk + i * 64, 64), 64)
            stream = tok[mine, :].astype(F32) + (CB[j, rows, :].astype(F32) + RZ[j, rows, :].astype(F32))
            n2[mine, :] = rms_scale(stream, ffn_gain[...]).astype(BF16)
            return 0

        lax.fori_loop(0, blk // 64, body, 0)
        ref = n2.at[row_block(j, t)]
        nb.extend(start([remote(ref, ref, n_s.at[j], n_r.at[j], s_dev)]))

    stream_block(0)
    step(6, 8)
    step(7)
    stream_block(1)
    arrived(3, 4, 5, 6)
    nb[0].wait_recv()

    def ffn_rows(j):
        def body(i, _):
            rows = pl.ds(pl.multiple_of(j * chip_rows + i * blk, blk), blk)
            x = n2[rows, :]
            full = hid // LANES
            for c in range(full):
                w = WG[:, :, 2 * c * LANES:2 * (c + 1) * LANES].reshape(width, 2 * LANES)
                zz = jnp.dot(x, w, preferred_element_type=F32)
                g, u = zz[:, :LANES], zz[:, LANES:]
                hidden[rows, c * LANES:(c + 1) * LANES] = (g / (1.0 + jnp.exp(-g)) * u).astype(BF16)
            rest = hid - full * LANES
            if rest:
                w = WG[:, :, 2 * full * LANES:].reshape(width, 2 * rest)
                zz = jnp.dot(x, w, preferred_element_type=F32)
                g, u = zz[:, :rest], zz[:, rest:]
                hidden[rows, full * LANES:] = (g / (1.0 + jnp.exp(-g)) * u).astype(BF16)
            return 0

        lax.fori_loop(0, chip_rows // blk, body, 0)

    ffn_rows(0)
    nb[1].wait_recv()
    ffn_rows(1)
    step(8)

    so, qo = [], []

    def down_send(k, s):
        for j in range(2):
            h = hidden[row_block(j, 1 - t), :]
            OS[s, j] = jnp.dot(h, WD[s], preferred_element_type=F32).astype(BF16)
        so.extend(start([remote(OS.at[s], RO.at[s], o_s.at[k], o_r.at[k], s_dev)]))
        for j in range(2):
            h = hidden[row_block(j, t), :]
            OW[s, j] = jnp.dot(h, WD[s], preferred_element_type=F32).astype(BF16)

    def down_pair(k, s):
        so[k].wait_recv()
        ZC[s] = (OW[s, 1 - p].astype(F32) + RO[s, 1 - p].astype(F32)).astype(BF16)
        qo.extend(start([remote(ZC.at[s], RF.at[s], q_s.at[k], q_r.at[k], z_dev)]))

    def finish(k, s):
        qo[k].wait_recv()
        cs = pl.ds(pl.multiple_of(s * cols, cols), cols)
        mine = row_block(p, t)
        stream = tok[mine, cs].astype(F32) + (CB[p, :, cs].astype(F32) + RZ[p, :, cs].astype(F32))
        branch = OW[s, p].astype(F32) + RO[s, p].astype(F32) + RF[s].astype(F32)
        out[:, cs] = (stream + branch).astype(BF16)

    slots = (f, x_of, y_of, d_of)
    down_send(0, slots[0])
    down_send(1, slots[1])
    down_pair(0, slots[0])
    down_send(2, slots[2])
    down_pair(1, slots[1])
    down_pair(2, slots[2])
    arrived(7, 8)
    down_send(3, slots[3])
    down_pair(3, slots[3])
    for k in range(4):
        finish(k, slots[k])
    for c in sent:
        c.wait_send()


def paired_local(
    tokens, mix_gain, w_gate_b, w_gate_c, w_conv_in, conv_taps, w_mix_out, ffn_gain,
    w_ffn_gate, w_ffn_up, w_ffn_down,
):
    chip_rows, width = tokens.shape
    n_fs = lax.axis_size("fs")
    rows_d = w_gate_b.shape[0]
    ch = w_gate_b.shape[1] // 2
    hid = w_ffn_gate.shape[1] // 2
    cols = w_mix_out.shape[1]
    blk = chip_rows // 2
    p = lax.rem(lax.axis_index("rep"), 2)
    half = [lax.dynamic_slice_in_dim(w, p * hid, hid, 1) for w in (w_ffn_gate, w_ffn_up)]
    parts = []
    for c in range(0, hid, LANES):
        parts += [h[:, c:c + LANES] for h in half]
    wgu = jnp.concatenate(parts, axis=1)

    VM = functools.partial(pltpu.VMEM, dtype=BF16)
    dma = lambda *s: pltpu.SemaphoreType.DMA(s)
    n_pieces = 9
    any_, vmem = pl.BlockSpec(memory_space=pl.ANY), pl.BlockSpec(memory_space=pltpu.VMEM)
    return pl.pallas_call(
        layer_kernel,
        out_shape=jax.ShapeDtypeStruct((blk, width), BF16),
        in_specs=[any_] * 7 + [vmem] * 3,
        out_specs=vmem,
        scratch_shapes=[
            pltpu.VMEM((2 * chip_rows, width), BF16),
            pltpu.VMEM((2 * chip_rows, width), BF16),
            pltpu.VMEM((2 * chip_rows, width), BF16),
            pltpu.VMEM((n_fs, rows_d, 3 * ch), BF16),
            pltpu.VMEM((n_fs, ch, cols), BF16),
            pltpu.VMEM((n_fs, rows_d, 2 * hid), BF16),
            pltpu.VMEM((n_fs, hid, cols), BF16),
            pltpu.VMEM((2 * chip_rows, ch), BF16),
            pltpu.VMEM((2 * chip_rows, width), BF16),
            pltpu.VMEM((2, blk, width), BF16),
            pltpu.VMEM((2, blk, width), BF16),
            pltpu.VMEM((2, blk, width), BF16),
            pltpu.VMEM((2 * chip_rows, hid), BF16),
            pltpu.VMEM((n_fs, 2, blk, cols), BF16),
            pltpu.VMEM((n_fs, 2, blk, cols), BF16),
            pltpu.VMEM((n_fs, 2, blk, cols), BF16),
            pltpu.VMEM((n_fs, blk, cols), BF16),
            pltpu.VMEM((n_fs, blk, cols), BF16),
            dma(7),
            dma(n_pieces, 2), dma(n_pieces, 2), dma(n_pieces, 2), dma(n_pieces, 2),
            dma(2), dma(2),
            dma(2), dma(2), dma(2), dma(2), dma(2), dma(2),
            dma(4), dma(4), dma(4), dma(4),
        ],
        compiler_params=pltpu.CompilerParams(
            collective_id=0, has_side_effects=True, vmem_limit_bytes=60 * 2**20
        ),
    )(
        tokens, w_gate_b, w_gate_c, w_conv_in, w_mix_out, wgu, w_ffn_down,
        mix_gain.reshape(1, width), conv_taps, ffn_gain.reshape(1, width),
    )


def causal_mix(product_in, conv_taps):
    shaped = product_in.reshape(product_in.shape[0] // LEN, LEN, product_in.shape[1])
    padded = jnp.pad(shaped, ((0, 0), (2, 0), (0, 0)))
    convolved = (
        conv_taps[0] * padded[:, :-2]
        + conv_taps[1] * padded[:, 1:-1]
        + conv_taps[2] * padded[:, 2:]
    )
    return convolved.reshape(product_in.shape)


def general_local(
    tokens, mix_gain, w_gate_b, w_gate_c, w_conv_in, conv_taps, w_mix_out, ffn_gain,
    w_ffn_gate, w_ffn_up, w_ffn_down,
):
    def scatter(product):
        return lax.psum_scatter(
            product.astype(BF16), "tp", scatter_dimension=0, tiled=True
        ).astype(F32)

    def dot(a, b):
        return jnp.dot(a, b, preferred_element_type=F32)

    def rows(w):
        return lax.all_gather(w, "fs", axis=0, tiled=True)

    normed = rms_scale(tokens.astype(F32), mix_gain).astype(BF16)
    gate_b, gate_c, conv_in = (dot(normed, rows(w)) for w in (w_gate_b, w_gate_c, w_conv_in))
    gated = (gate_b * causal_mix(gate_c * conv_in, conv_taps)).astype(BF16)
    row_count = normed.shape[0] // lax.axis_size("tp")
    branch = scatter(dot(gated, lax.all_gather(w_mix_out, "fs", axis=1, tiled=True)))
    own = lax.dynamic_slice_in_dim(tokens, lax.axis_index("tp") * row_count, row_count, 0)
    stream = own.astype(F32) + branch
    normed_two = lax.all_gather(
        rms_scale(stream, ffn_gain).astype(BF16), "tp", axis=0, tiled=True
    )
    hidden = (jax.nn.silu(dot(normed_two, rows(w_ffn_gate))) * dot(normed_two, rows(w_ffn_up))).astype(BF16)
    ffn_branch = scatter(dot(hidden, lax.all_gather(w_ffn_down, "fs", axis=1, tiled=True)))
    return (stream + ffn_branch).astype(BF16)


def solution(mesh):
    in_specs = (
        P(("rep", "fs"), None),
        P(),
        P("fs", "tp"),
        P("fs", "tp"),
        P("fs", "tp"),
        P(None, "tp"),
        P("tp", "fs"),
        P(),
        P("fs", "tp"),
        P("fs", "tp"),
        P("tp", "fs"),
    )
    out_specs = P(("rep", "fs", "tp"), None)
    size = mesh.shape
    paired = size["tp"] == 2 and size["fs"] == 4 and size["rep"] % 2 == 0
    body = paired_local if paired else general_local
    return jax.shard_map(body, mesh=mesh, in_specs=in_specs, out_specs=out_specs, check_vma=False)
```

```python
import jax
import jax.numpy as jnp
from jax import lax
from jax.experimental import pallas as pl
from jax.experimental.pallas import tpu as pltpu
from jax.sharding import PartitionSpec as P

LEN = 128
LANES = 128
EPSILON = 1e-06
MESH = pl.DeviceIdType.MESH
F32 = jnp.float32
BF16 = jnp.bfloat16


def rms_scale(values, gain):
    return values * lax.rsqrt(jnp.mean(values * values, axis=-1, keepdims=True) + EPSILON) * gain


N_CHUNKS = 4
PIECES = (2, 1, 4, 2)


def layer_kernel(
    tokens, wb, wc, wi, wm_in, wg_in, wu_in, wd_in, mix_gain, taps, ffn_gain,
    out,
    tok, normed, n2, WA, WM, WG, WD, tile, gated, MP, RS, CB, RZ, hidden, OP, RO, ZC, RF,
    load_sem, ds, dr, fs_, fr, tz_s, tz_r, ts_s, ts_r, sib_s, sib_r, z_s, z_r, n_s, n_r,
    o_s, o_r, q_s, q_r,
):
    n_fs, rows_d, _ = WA.shape
    ch = gated.shape[1]
    hid = hidden.shape[1]
    width = tokens.shape[1]
    half = tokens.shape[0] // 4
    cols = WM.shape[2]
    full, rest = hid // LANES, hid % LANES

    r = lax.axis_index("rep")
    f = lax.axis_index("fs")
    t = lax.axis_index("tp")
    p = lax.rem(r, 2)
    z_dev = {"rep": r + 1 - 2 * p}
    x_of = f + 1 - 2 * lax.rem(f, 2)
    y_of = lax.rem(f + 2, 4)
    d_of = lax.rem(x_of + 2, 4)
    x_dev, y_dev, s_dev = {"fs": x_of}, {"fs": y_of}, {"tp": 1 - t}

    def part(c, core):
        return pl.ds(pl.multiple_of((2 * c + core) * half, half), half)

    def chunk(c):
        return pl.ds(pl.multiple_of(2 * c * half, 2 * half), 2 * half)

    chan = pl.ds(pl.multiple_of(p * ch, ch), ch)
    loads = []

    def load(src, dst):
        c = pltpu.make_async_copy(src, dst, load_sem.at[len(loads)])
        c.start()
        loads.append(c)
        return c

    l_wa = [load(w.at[:, chan], WA.at[f, :, pl.ds(i * ch, ch)]) for i, w in enumerate((wb, wc, wi))]
    l_tok = [
        load(tokens.at[pl.ds((2 * core + h) * half, half)], tok.at[part(2 * h + p, core)])
        for h in range(2) for core in range(2)
    ]
    l_rest = [load(wm_in.at[chan, :], WM.at[f])]
    far = (full + (1 if rest else 0)) * LANES
    for i, w in enumerate((wg_in, wu_in)):
        for c in range(full):
            col = pl.ds(pl.multiple_of(p * far + c * LANES, LANES), LANES)
            l_rest.append(load(w.at[:, col], WG.at[f, :, pl.ds((2 * c + i) * LANES, LANES)]))
        if rest:
            l_rest.append(load(w.at[:, pl.ds(full * LANES, LANES)], tile.at[i]))
    aligned = full * LANES
    l_rest.append(load(wd_in.at[pl.ds(pl.multiple_of(p * far, LANES), aligned)], WD.at[f, pl.ds(0, aligned)]))
    if rest:
        l_rest.append(load(
            wd_in.at[pl.ds(pl.multiple_of(aligned + p * rest, rest), rest)],
            WD.at[f, pl.ds(aligned, rest)],
        ))

    barrier = pltpu.get_barrier_semaphore()
    for dev in (x_dev, y_dev, z_dev, s_dev):
        pl.semaphore_signal(barrier, inc=1, device_id=dev, device_id_type=MESH)
    pl.semaphore_wait(barrier, 4)

    def remote(src, dst, s, rcv, dev):
        return pltpu.make_async_remote_copy(
            src_ref=src, dst_ref=dst, send_sem=s, recv_sem=rcv, device_id=dev, device_id_type=MESH
        )

    pieces = []
    for buf, parts in zip((WA, WM, WG, WD), PIECES):
        n = buf.shape[1] // parts
        pieces += [(buf, i * n, n) for i in range(parts)]

    def direct(k):
        buf, r0, n = pieces[k]
        ref = buf.at[f, pl.ds(r0, n)]
        return [remote(ref, ref, ds.at[k, c], dr.at[k, c], dev) for c, dev in ((0, x_dev), (1, y_dev))]

    def forward(k):
        buf, r0, n = pieces[k]
        a = buf.at[x_of, pl.ds(r0, n // 2)]
        b = buf.at[y_of, pl.ds(r0 + n // 2, n // 2)]
        return [
            remote(b, b, fs_.at[k, 0], fr.at[k, 0], x_dev),
            remote(a, a, fs_.at[k, 1], fr.at[k, 1], y_dev),
        ]

    sent = []

    def start(*copies):
        for c in copies:
            c.start()
            sent.append(c)
        return copies

    D, F = {}, {}

    def send(*ks):
        for k in ks:
            D[k] = start(*direct(k))

    def step(k, *more):
        for c in D[k]:
            c.wait_recv()
        F[k] = start(*forward(k))
        send(*more)

    def arrived(*ks):
        for k in ks:
            for c in F[k]:
                c.wait_recv()

    for c in l_wa:
        c.wait()
    send(0, 1)
    for c in l_tok:
        c.wait()
    tz, ts = [], []
    for h in range(2):
        ref = tok.at[part(2 * h + p, t)]
        tz += start(remote(ref, ref, tz_s.at[h], tz_r.at[h], z_dev))

    def relay(h):
        tz[h].wait_recv()
        ref = tok.at[part(2 * h + 1 - p, t)]
        ts.extend(start(remote(ref, ref, ts_s.at[h], ts_r.at[h], s_dev)))

    def norm_chunk(c):
        def body(i, _):
            rows = pl.ds(pl.multiple_of(2 * c * half + i * 64, 64), 64)
            normed[rows, :] = rms_scale(tok[rows, :].astype(F32), mix_gain[...]).astype(BF16)
            return 0

        lax.fori_loop(0, 2 * half // 64, body, 0)

    norm_chunk(p)
    norm_chunk(2 + p)
    for c in l_rest:
        c.wait()
    if rest:
        gate, up = tile[0].astype(F32), tile[1].astype(F32)
        lane = lax.broadcasted_iota(jnp.int32, gate.shape, 1)
        low = jnp.where(lane < rest, gate, pltpu.roll(up, rest, 1))
        high = jnp.where(lane < rest, pltpu.roll(gate, rest, 1), up)
        WG[f, :, 2 * aligned:] = jnp.where(p == 0, low, high).astype(BF16)
    step(0, 2)
    relay(0)
    step(1)
    ts[0].wait_recv()
    norm_chunk(1 - p)
    relay(1)
    step(2, 3, 4)
    ts[1].wait_recv()
    norm_chunk(3 - p)
    arrived(0, 1)

    tap = [taps[pl.ds(i, 1), chan] for i in range(3)]
    pos = lax.rem(lax.broadcasted_iota(jnp.int32, (2 * half, ch), 0), LEN)

    def mix_in(c):
        x = normed[chunk(c), :]

        def proj(q):
            w = WA[:, :, q * ch:(q + 1) * ch].reshape(width, ch)
            return jnp.dot(x, w, preferred_element_type=F32)

        pr = proj(1) * proj(2)
        one = jnp.where(pos >= 1, pltpu.roll(pr, 1, 0), 0.0)
        two = jnp.where(pos >= 2, pltpu.roll(pr, 2, 0), 0.0)
        conv = tap[0] * two + tap[1] * one + tap[2] * pr
        gated[chunk(c), :] = (proj(0) * conv).astype(BF16)

    sib, zc, nb = [], [], []

    def mix_out(c):
        g = gated[chunk(c), :]
        for s in range(n_fs):
            MP[chunk(c), s * cols:(s + 1) * cols] = jnp.dot(
                g, WM[s], preferred_element_type=F32
            ).astype(BF16)
        sib.extend(start(remote(MP.at[part(c, 1 - t)], RS.at[c], sib_s.at[c], sib_r.at[c], s_dev)))

    def mix_pair(c):
        sib[c].wait_recv()
        CB[c] = (MP[part(c, t), :].astype(F32) + RS[c].astype(F32)).astype(BF16)
        zc.extend(start(remote(CB.at[c], RZ.at[c], z_s.at[c], z_r.at[c], z_dev)))

    mix_in(0)
    mix_in(1)
    arrived(2)
    mix_out(0)
    mix_out(1)
    mix_pair(0)
    mix_in(2)
    mix_out(2)
    mix_pair(1)
    mix_in(3)
    mix_out(3)
    mix_pair(2)
    mix_pair(3)

    def stream_chunk(c):
        zc[c].wait_recv()
        step_rows = 32

        def body(i, _):
            rows = pl.ds(pl.multiple_of(i * step_rows, step_rows), step_rows)
            mine = pl.ds(pl.multiple_of((2 * c + t) * half + i * step_rows, step_rows), step_rows)
            stream = tok[mine, :].astype(F32) + (CB[c, rows, :].astype(F32) + RZ[c, rows, :].astype(F32))
            n2[mine, :] = rms_scale(stream, ffn_gain[...]).astype(BF16)
            return 0

        lax.fori_loop(0, half // step_rows, body, 0)
        ref = n2.at[part(c, t)]
        nb.extend(start(remote(ref, ref, n_s.at[c], n_r.at[c], s_dev)))

    def ffn_chunks(lo, hi):
        for c in range(lo, hi):
            nb[c].wait_recv()

        def body(c, _):
            rows = chunk(c)
            x = n2[rows, :]
            for k in range(0, hid, LANES):
                n = min(LANES, hid - k)
                w = WG[:, :, 2 * k:2 * (k + n)].reshape(width, 2 * n)
                zz = jnp.dot(x, w, preferred_element_type=F32)
                g, u = zz[:, :n], zz[:, n:]
                hidden[rows, k:k + n] = (g / (1.0 + jnp.exp(-g)) * u).astype(BF16)
            return 0

        lax.fori_loop(lo, hi, body, 0)

    step(3, 5)
    step(4, 6)
    stream_chunk(0)
    step(5)
    stream_chunk(1)
    step(6, 7, 8)
    stream_chunk(2)
    arrived(3, 4, 5, 6)
    ffn_chunks(0, 3)
    stream_chunk(3)
    ffn_chunks(3, 4)

    so, qo = [], []

    def down_send(k, s):
        def body(c, _):
            both = jnp.dot(hidden[chunk(c), :], WD[s], preferred_element_type=F32).astype(BF16)
            OP[s, 0, c] = both[:half]
            OP[s, 1, c] = both[half:]
            return 0

        lax.fori_loop(0, N_CHUNKS, body, 0)
        so.extend(start(remote(OP.at[s, 1 - t], RO.at[s], o_s.at[k], o_r.at[k], s_dev)))

    def down_pair(k, s):
        so[k].wait_recv()
        for h in range(2):
            c = 2 * h + 1 - p
            ZC[s, h] = (OP[s, t, c].astype(F32) + RO[s, c].astype(F32)).astype(BF16)
        qo.extend(start(remote(ZC.at[s], RF.at[s], q_s.at[k], q_r.at[k], z_dev)))

    def finish(k, s):
        qo[k].wait_recv()
        cs = pl.ds(pl.multiple_of(s * cols, cols), cols)
        for h in range(2):
            c = 2 * h + p
            stream = tok[part(c, t), cs].astype(F32) + (CB[c, :, cs].astype(F32) + RZ[c, :, cs].astype(F32))
            branch = OP[s, t, c].astype(F32) + RO[s, c].astype(F32) + RF[s, h].astype(F32)
            out[h * half:(h + 1) * half, cs] = (stream + branch).astype(BF16)

    slots = (f, x_of, y_of, d_of)
    down_send(0, slots[0])
    step(7)
    down_pair(0, slots[0])
    step(8)
    down_send(1, slots[1])
    down_send(2, slots[2])
    down_pair(1, slots[1])
    down_pair(2, slots[2])
    arrived(7, 8)
    down_send(3, slots[3])
    finish(0, slots[0])
    down_pair(3, slots[3])
    for k in range(1, 4):
        finish(k, slots[k])
    for c in sent:
        c.wait_send()


def paired_local(
    tokens, mix_gain, w_gate_b, w_gate_c, w_conv_in, conv_taps, w_mix_out, ffn_gain,
    w_ffn_gate, w_ffn_up, w_ffn_down,
):
    chip_rows, width = tokens.shape
    n_fs = lax.axis_size("fs")
    rows_d = w_gate_b.shape[0]
    ch = w_gate_b.shape[1] // 2
    hid = w_ffn_gate.shape[1] // 2
    cols = w_mix_out.shape[1]
    half = chip_rows // 4
    group = 2 * chip_rows
    n_pieces = sum(PIECES)
    n_loads = 16 + 2 * (hid // LANES)

    def vmem(*shape):
        return pltpu.VMEM(shape, BF16)

    def dma(*shape):
        return pltpu.SemaphoreType.DMA(shape)

    return pl.pallas_call(
        layer_kernel,
        out_shape=jax.ShapeDtypeStruct((2 * half, width), BF16),
        in_specs=[pl.BlockSpec(memory_space=pl.ANY)] * 8 + [pl.BlockSpec(memory_space=pltpu.VMEM)] * 3,
        out_specs=pl.BlockSpec(memory_space=pltpu.VMEM),
        scratch_shapes=[
            vmem(group, width),
            vmem(group, width),
            vmem(group, width),
            vmem(n_fs, rows_d, 3 * ch),
            vmem(n_fs, ch, cols),
            vmem(n_fs, rows_d, 2 * hid),
            vmem(n_fs, hid, cols),
            vmem(2, rows_d, LANES),
            vmem(group, ch),
            vmem(group, width),
            vmem(N_CHUNKS, half, width),
            vmem(N_CHUNKS, half, width),
            vmem(N_CHUNKS, half, width),
            vmem(group, hid),
            vmem(n_fs, 2, N_CHUNKS, half, cols),
            vmem(n_fs, N_CHUNKS, half, cols),
            vmem(n_fs, 2, half, cols),
            vmem(n_fs, 2, half, cols),
            dma(n_loads),
            *[dma(n_pieces, 2)] * 4,
            *[dma(2)] * 4,
            *[dma(N_CHUNKS)] * 6,
            *[dma(n_fs)] * 4,
        ],
        compiler_params=pltpu.CompilerParams(
            collective_id=0, has_side_effects=True, vmem_limit_bytes=60 * 2**20
        ),
    )(
        tokens, w_gate_b, w_gate_c, w_conv_in, w_mix_out, w_ffn_gate, w_ffn_up, w_ffn_down,
        mix_gain.reshape(1, width), conv_taps, ffn_gain.reshape(1, width),
    )


def causal_mix(product_in, conv_taps):
    shaped = product_in.reshape(product_in.shape[0] // LEN, LEN, product_in.shape[1])
    padded = jnp.pad(shaped, ((0, 0), (2, 0), (0, 0)))
    convolved = (
        conv_taps[0] * padded[:, :-2]
        + conv_taps[1] * padded[:, 1:-1]
        + conv_taps[2] * padded[:, 2:]
    )
    return convolved.reshape(product_in.shape)


def general_local(
    tokens, mix_gain, w_gate_b, w_gate_c, w_conv_in, conv_taps, w_mix_out, ffn_gain,
    w_ffn_gate, w_ffn_up, w_ffn_down,
):
    def scatter(product):
        return lax.psum_scatter(
            product.astype(BF16), "tp", scatter_dimension=0, tiled=True
        ).astype(F32)

    def dot(a, b):
        return jnp.dot(a, b, preferred_element_type=F32)

    def rows(w):
        return lax.all_gather(w, "fs", axis=0, tiled=True)

    normed = rms_scale(tokens.astype(F32), mix_gain).astype(BF16)
    gate_b, gate_c, conv_in = (dot(normed, rows(w)) for w in (w_gate_b, w_gate_c, w_conv_in))
    gated = (gate_b * causal_mix(gate_c * conv_in, conv_taps)).astype(BF16)
    row_count = normed.shape[0] // lax.axis_size("tp")
    branch = scatter(dot(gated, lax.all_gather(w_mix_out, "fs", axis=1, tiled=True)))
    own = lax.dynamic_slice_in_dim(tokens, lax.axis_index("tp") * row_count, row_count, 0)
    stream = own.astype(F32) + branch
    normed_two = lax.all_gather(
        rms_scale(stream, ffn_gain).astype(BF16), "tp", axis=0, tiled=True
    )
    hidden = (jax.nn.silu(dot(normed_two, rows(w_ffn_gate))) * dot(normed_two, rows(w_ffn_up))).astype(BF16)
    ffn_branch = scatter(dot(hidden, lax.all_gather(w_ffn_down, "fs", axis=1, tiled=True)))
    return (stream + ffn_branch).astype(BF16)


def solution(mesh):
    in_specs = (
        P(("rep", "fs"), None),
        P(),
        P("fs", "tp"),
        P("fs", "tp"),
        P("fs", "tp"),
        P(None, "tp"),
        P("tp", "fs"),
        P(),
        P("fs", "tp"),
        P("fs", "tp"),
        P("tp", "fs"),
    )
    out_specs = P(("rep", "fs", "tp"), None)
    size = mesh.shape
    square = size["tp"] == 2 and size["fs"] == 4 and size["rep"] % 2 == 0

    def local(*arrays):
        rows, width = arrays[0].shape
        channels, hidden = arrays[2].shape[1], arrays[8].shape[1]
        fits = (
            square
            and rows % (4 * LEN) == 0
            and channels % (2 * LANES) == 0
            and hidden % LANES == 0
            and width % (4 * LANES) == 0
        )
        return (paired_local if fits else general_local)(*arrays)

    return jax.shard_map(local, mesh=mesh, in_specs=in_specs, out_specs=out_specs, check_vma=False)
```

```python
import jax
import jax.numpy as jnp
from jax import lax
from jax.experimental import pallas as pl
from jax.experimental.pallas import tpu as pltpu
from jax.sharding import PartitionSpec as P

LEN = 128
LANES = 128
EPSILON = 1e-06
MESH = pl.DeviceIdType.MESH
F32 = jnp.float32
BF16 = jnp.bfloat16


def rms_scale(values, gain):
    return values * lax.rsqrt(jnp.mean(values * values, axis=-1, keepdims=True) + EPSILON) * gain


N_CHUNKS = 4


def weight_pieces(rows_d, n_conv, n_mix, n_gate_up, n_down, mix_rows, down_rows):
    pieces = [(0, i * rows_d // 2, rows_d // 2, 0, n_conv) for i in range(2)]
    pieces.append((1, 0, mix_rows, 0, n_mix))
    units = n_gate_up // (2 * LANES)
    gate_up = sorted({2 * LANES * u for u in (2 * units // 5, 4 * units // 5, units)} | {0, n_gate_up})
    down = (0, n_down // 2, 3 * n_down // 4, n_down)
    for weight, rows, cuts in ((2, rows_d, gate_up), (3, down_rows, down)):
        pieces += [(weight, 0, rows, a, b - a) for a, b in zip(cuts, cuts[1:])]
    return pieces


def layer_kernel(
    tokens, wb, wc, wi, wm_in, wg_in, wu_in, wd_in, mix_gain, taps, ffn_gain,
    out,
    tok, normed, n2, WA, WM, WG, WD, tile, gated, MP, RS, BR, hidden, OP, RO, ZC, RF,
    load_sem, ds, dr, fs_, fr, tz_s, tz_r, ts_s, ts_r, g_s, g_r, sib_s, sib_r, z_s, z_r, n_s, n_r,
    o_s, o_r, q_s, q_r,
):
    n_fs, rows_d, _ = WA.shape
    ch = gated.shape[2]
    hid = hidden.shape[1]
    width = tokens.shape[1]
    half = tokens.shape[0] // 4
    cols = WD.shape[2]
    mcols = WM.shape[2]
    full, rest = hid // LANES, hid % LANES

    r = lax.axis_index("rep")
    f = lax.axis_index("fs")
    t = lax.axis_index("tp")
    p = lax.rem(r, 2)
    z_dev = {"rep": r + 1 - 2 * p}
    x_of = f + 1 - 2 * lax.rem(f, 2)
    y_of = lax.rem(f + 2, 4)
    d_of = lax.rem(x_of + 2, 4)
    x_dev, y_dev, s_dev = {"fs": x_of}, {"fs": y_of}, {"tp": 1 - t}

    def part(c, core):
        return pl.ds(pl.multiple_of((2 * c + core) * half, half), half)

    def chunk(c):
        return pl.ds(pl.multiple_of(2 * c * half, 2 * half), 2 * half)

    chan = pl.ds(pl.multiple_of(p * ch, ch), ch)
    loads = []

    def load(src, dst):
        c = pltpu.make_async_copy(src, dst, load_sem.at[len(loads)])
        c.start()
        loads.append(c)
        return c

    l_wa = []
    for k in range(2):
        rows = pl.ds(k * (rows_d // 2), rows_d // 2)
        l_wa.append([
            load(w.at[rows, chan], WA.at[f, rows, pl.ds(i * ch, ch)]) for i, w in enumerate((wb, wc, wi))
        ])
    l_tok = [
        load(tokens.at[pl.ds((2 * core + h) * half, half)], tok.at[part(2 * h + p, core)])
        for h in range(2) for core in range(2)
    ]
    barrier = pltpu.get_barrier_semaphore()
    for dev in (x_dev, y_dev, z_dev, s_dev):
        pl.semaphore_signal(barrier, inc=1, device_id=dev, device_id_type=MESH)
    pl.semaphore_wait(barrier, 4)

    def remote(src, dst, s, rcv, dev):
        return pltpu.make_async_remote_copy(
            src_ref=src, dst_ref=dst, send_sem=s, recv_sem=rcv, device_id=dev, device_id_type=MESH
        )

    bufs = (WA, WM, WG, WD)
    pieces = weight_pieces(rows_d, 3 * ch, mcols, 2 * hid, cols, WM.shape[1], hid)

    def cut(k, slot, first, parts):
        w, r0, n, c0, nc = pieces[k]
        return bufs[w].at[slot, pl.ds(r0 + first * n // 2, parts * n // 2), pl.ds(c0, nc)]

    def direct(k):
        ref = cut(k, f, 0, 2)
        return [remote(ref, ref, ds.at[k, c], dr.at[k, c], dev) for c, dev in ((0, x_dev), (1, y_dev))]

    def forward(k):
        a, b = cut(k, x_of, 0, 1), cut(k, y_of, 1, 1)
        return [
            remote(b, b, fs_.at[k, 0], fr.at[k, 0], x_dev),
            remote(a, a, fs_.at[k, 1], fr.at[k, 1], y_dev),
        ]

    sent = []

    def start(*copies):
        for c in copies:
            c.start()
            sent.append(c)
        return copies

    D, F = {}, {}

    def send(*ks):
        for k in ks:
            D[k] = start(*direct(k))

    def step(k, *more):
        for c in D[k]:
            c.wait_recv()
        F[k] = start(*forward(k))
        send(*more)

    def arrived(*ks):
        for k in ks:
            for c in F[k]:
                c.wait_recv()

    for k in range(2):
        for c in l_wa[k]:
            c.wait()
        send(k)
    for c in l_tok:
        c.wait()
    tz, ts = [], []
    for h in range(2):
        ref = tok.at[part(2 * h + p, t)]
        tz += start(remote(ref, ref, tz_s.at[h], tz_r.at[h], z_dev))

    def relay(h):
        tz[h].wait_recv()
        ref = tok.at[part(2 * h + 1 - p, t)]
        ts.extend(start(remote(ref, ref, ts_s.at[h], ts_r.at[h], s_dev)))

    def norm_chunk(c):
        def body(i, _):
            rows = pl.ds(pl.multiple_of(2 * c * half + i * 64, 64), 64)
            normed[rows, :] = rms_scale(tok[rows, :].astype(F32), mix_gain[...]).astype(BF16)
            return 0

        lax.fori_loop(0, 2 * half // 64, body, 0)

    l_rest = [load(wm_in.at[:, pl.ds(pl.multiple_of(p * mcols, mcols), mcols)], WM.at[f])]
    far = (full + (1 if rest else 0)) * LANES
    for i, w in enumerate((wg_in, wu_in)):
        for c in range(full):
            col = pl.ds(pl.multiple_of(p * far + c * LANES, LANES), LANES)
            l_rest.append(load(w.at[:, col], WG.at[f, :, pl.ds((2 * c + i) * LANES, LANES)]))
        if rest:
            l_rest.append(load(w.at[:, pl.ds(full * LANES, LANES)], tile.at[i]))
    aligned = full * LANES
    l_rest.append(load(wd_in.at[pl.ds(pl.multiple_of(p * far, LANES), aligned)], WD.at[f, pl.ds(0, aligned)]))
    if rest:
        l_rest.append(load(
            wd_in.at[pl.ds(pl.multiple_of(aligned + p * rest, rest), rest)],
            WD.at[f, pl.ds(aligned, rest)],
        ))


    norm_chunk(p)
    norm_chunk(2 + p)
    for c in l_rest:
        c.wait()
    if rest:
        gate, up = tile[0].astype(F32), tile[1].astype(F32)
        lane = lax.broadcasted_iota(jnp.int32, gate.shape, 1)
        low = jnp.where(lane < rest, gate, pltpu.roll(up, rest, 1))
        high = jnp.where(lane < rest, pltpu.roll(gate, rest, 1), up)
        WG[f, :, 2 * aligned:] = jnp.where(p == 0, low, high).astype(BF16)
    step(0, 2)
    relay(0)
    step(1)
    ts[0].wait_recv()
    norm_chunk(1 - p)
    relay(1)
    step(2, 3, 4)
    ts[1].wait_recv()
    norm_chunk(3 - p)
    arrived(0, 1)

    tap = [taps[pl.ds(i, 1), chan] for i in range(3)]
    pos = lax.rem(lax.broadcasted_iota(jnp.int32, (2 * half, ch), 0), LEN)

    def mix_in(c):
        x = normed[chunk(c), :]

        def proj(q):
            w = WA[:, :, q * ch:(q + 1) * ch].reshape(width, ch)
            return jnp.dot(x, w, preferred_element_type=F32)

        pr = proj(1) * proj(2)
        one = jnp.where(pos >= 1, pltpu.roll(pr, 1, 0), 0.0)
        two = jnp.where(pos >= 2, pltpu.roll(pr, 2, 0), 0.0)
        conv = tap[0] * two + tap[1] * one + tap[2] * pr
        gated[p, chunk(c), :] = (proj(0) * conv).astype(BF16)
        ref = gated.at[p, chunk(c)]
        gz.extend(start(remote(ref, ref, g_s.at[c], g_r.at[c], z_dev)))

    gz, sib, zc, nb = [], [], [], []

    def mix_out(c):
        gz[c].wait_recv()
        g = jnp.concatenate([gated[0, chunk(c), :], gated[1, chunk(c), :]], axis=1)
        for s in range(n_fs):
            MP[chunk(c), s * mcols:(s + 1) * mcols] = jnp.dot(
                g, WM[s], preferred_element_type=F32
            ).astype(BF16)
        sib.extend(start(remote(MP.at[part(c, 1 - t)], RS.at[c], sib_s.at[c], sib_r.at[c], s_dev)))

    def mix_pair(c):
        sib[c].wait_recv()
        BR[p, c] = (MP[part(c, t), :].astype(F32) + RS[c].astype(F32)).astype(BF16)
        zc.extend(start(remote(BR.at[p, c], BR.at[p, c], z_s.at[c], z_r.at[c], z_dev)))

    for c in range(N_CHUNKS):
        mix_in(c)
    arrived(2)
    mix_out(0)
    for c in range(1, N_CHUNKS):
        mix_out(c)
        mix_pair(c - 1)
    mix_pair(N_CHUNKS - 1)

    def stream_chunk(c):
        zc[c].wait_recv()
        step_rows = 32

        def body(i, _):
            rows = pl.ds(pl.multiple_of(i * step_rows, step_rows), step_rows)
            mine = pl.ds(pl.multiple_of((2 * c + t) * half + i * step_rows, step_rows), step_rows)
            branch = jnp.concatenate(
                [BR[q, c, rows, s * mcols:(s + 1) * mcols] for s in range(n_fs) for q in range(2)], axis=1
            )
            stream = tok[mine, :].astype(F32) + branch.astype(F32)
            n2[mine, :] = rms_scale(stream, ffn_gain[...]).astype(BF16)
            return 0

        lax.fori_loop(0, half // step_rows, body, 0)
        ref = n2.at[part(c, t)]
        nb.extend(start(remote(ref, ref, n_s.at[c], n_r.at[c], s_dev)))

    def ffn_piece(k):
        arrived(k)
        _, _, _, c0, nc = pieces[k]

        def body(i, _):
            rows = pl.ds(pl.multiple_of(4 * i * half, 4 * half), 4 * half)
            x = n2[rows, :]
            for a in range(c0, c0 + nc, 2 * LANES):
                n = min(2 * LANES, c0 + nc - a) // 2
                w = WG[:, :, a:a + 2 * n].reshape(width, 2 * n)
                zz = jnp.dot(x, w, preferred_element_type=F32)
                g, u = zz[:, :n], zz[:, n:]
                hidden[rows, a // 2:a // 2 + n] = (g / (1.0 + jnp.exp(-g)) * u).astype(BF16)
            return 0

        lax.fori_loop(0, N_CHUNKS // 2, body, 0)

    step(3, 5)
    stream_chunk(0)
    stream_chunk(1)
    step(4, 6)
    stream_chunk(2)
    stream_chunk(3)
    for c in nb:
        c.wait_recv()
    ffn_piece(3)
    step(5)
    ffn_piece(4)
    step(6, 7, 8)
    ffn_piece(5)
    ffn_piece(6)

    cuts = [pieces[k][3:] for k in (7, 8, 9)]
    blocks = [(f, 0, cols)]
    blocks += [(x_of, *cuts[0]), (y_of, *cuts[0])]
    blocks += [(x_of, *cuts[1]), (y_of, *cuts[1]), (d_of, *cuts[0])]
    blocks += [(x_of, *cuts[2]), (y_of, *cuts[2]), (d_of, *cuts[1]), (d_of, *cuts[2])]
    so, qo = [], []

    def down_send(*ks):
        for k in ks:
            s, c0, nc = blocks[k]
            cs = pl.ds(c0, nc)

            def body(i, _, s=s, c0=c0, nc=nc):
                rows = pl.ds(pl.multiple_of(4 * i * half, 4 * half), 4 * half)
                prod = jnp.dot(
                    hidden[rows, :], WD[s, :, c0:c0 + nc], preferred_element_type=F32
                ).astype(BF16)
                for e in range(4):
                    OP[s, e % 2, 2 * i + e // 2, :, c0:c0 + nc] = prod[e * half:(e + 1) * half]
                return 0

            lax.fori_loop(0, N_CHUNKS // 2, body, 0)
            so.extend(start(remote(
                OP.at[s, 1 - t, :, :, cs], RO.at[s, :, :, cs], o_s.at[k], o_r.at[k], s_dev
            )))

    def down_pair(*ks):
        for k in ks:
            so[k].wait_recv()
            s, c0, nc = blocks[k]
            cs = pl.ds(c0, nc)
            for h in range(2):
                c = 2 * h + 1 - p
                ZC[s, h, :, cs] = (OP[s, t, c, :, cs].astype(F32) + RO[s, c, :, cs].astype(F32)).astype(BF16)
            qo.extend(start(remote(
                ZC.at[s, :, :, cs], RF.at[s, :, :, cs], q_s.at[k], q_r.at[k], z_dev
            )))

    def finish(*ks):
        for k in ks:
            qo[k].wait_recv()
            s, c0, nc = blocks[k]
            for a in range(0, nc, LANES):
                lo = c0 + a
                q, at = lo // mcols, lo % mcols
                cs = pl.ds(lo, LANES)
                ms = pl.ds(pl.multiple_of(s * mcols + at, LANES), LANES)
                whole = pl.ds(pl.multiple_of(s * cols + lo, LANES), LANES)
                for h in range(2):
                    c = 2 * h + p
                    stream = tok[part(c, t), whole].astype(F32) + BR[q, c, :, ms].astype(F32)
                    branch = (
                        OP[s, t, c, :, cs].astype(F32)
                        + RO[s, c, :, cs].astype(F32)
                        + RF[s, h, :, cs].astype(F32)
                    )
                    out[h * half:(h + 1) * half, whole] = (stream + branch).astype(BF16)

    down_send(0)
    step(7, 9)
    down_pair(0)
    down_send(1, 2)
    down_pair(1, 2)
    step(8)
    down_send(3, 4)
    down_pair(3, 4)
    arrived(7)
    down_send(5)
    step(9)
    down_pair(5)
    down_send(6, 7)
    down_pair(6, 7)
    finish(0, 1, 2)
    arrived(8)
    down_send(8)
    down_pair(8)
    finish(3, 4)
    arrived(9)
    down_send(9)
    down_pair(9)
    finish(5, 6, 7, 8, 9)
    for c in sent:
        c.wait_send()


def paired_local(
    tokens, mix_gain, w_gate_b, w_gate_c, w_conv_in, conv_taps, w_mix_out, ffn_gain,
    w_ffn_gate, w_ffn_up, w_ffn_down,
):
    chip_rows, width = tokens.shape
    n_fs = lax.axis_size("fs")
    rows_d = w_gate_b.shape[0]
    ch = w_gate_b.shape[1] // 2
    hid = w_ffn_gate.shape[1] // 2
    cols = w_mix_out.shape[1]
    half = chip_rows // 4
    group = 2 * chip_rows
    n_pieces = len(weight_pieces(rows_d, 3 * ch, cols // 2, 2 * hid, cols, 2 * ch, hid))
    n_blocks = 10
    n_loads = 20 + 2 * (hid // LANES)

    def vmem(*shape):
        return pltpu.VMEM(shape, BF16)

    def dma(*shape):
        return pltpu.SemaphoreType.DMA(shape)

    return pl.pallas_call(
        layer_kernel,
        out_shape=jax.ShapeDtypeStruct((2 * half, width), BF16),
        in_specs=[pl.BlockSpec(memory_space=pl.ANY)] * 8 + [pl.BlockSpec(memory_space=pltpu.VMEM)] * 3,
        out_specs=pl.BlockSpec(memory_space=pltpu.VMEM),
        scratch_shapes=[
            vmem(group, width),
            vmem(group, width),
            vmem(group, width),
            vmem(n_fs, rows_d, 3 * ch),
            vmem(n_fs, 2 * ch, cols // 2),
            vmem(n_fs, rows_d, 2 * hid),
            vmem(n_fs, hid, cols),
            vmem(2, rows_d, LANES),
            vmem(2, group, ch),
            vmem(group, width // 2),
            vmem(N_CHUNKS, half, width // 2),
            vmem(2, N_CHUNKS, half, width // 2),
            vmem(group, hid),
            vmem(n_fs, 2, N_CHUNKS, half, cols),
            vmem(n_fs, N_CHUNKS, half, cols),
            vmem(n_fs, 2, half, cols),
            vmem(n_fs, 2, half, cols),
            dma(n_loads),
            *[dma(n_pieces, 2)] * 4,
            *[dma(2)] * 4,
            *[dma(N_CHUNKS)] * 8,
            *[dma(n_blocks)] * 4,
        ],
        compiler_params=pltpu.CompilerParams(
            collective_id=0, has_side_effects=True, vmem_limit_bytes=60 * 2**20
        ),
    )(
        tokens, w_gate_b, w_gate_c, w_conv_in, w_mix_out, w_ffn_gate, w_ffn_up, w_ffn_down,
        mix_gain.reshape(1, width), conv_taps, ffn_gain.reshape(1, width),
    )


def causal_mix(product_in, conv_taps):
    shaped = product_in.reshape(product_in.shape[0] // LEN, LEN, product_in.shape[1])
    padded = jnp.pad(shaped, ((0, 0), (2, 0), (0, 0)))
    convolved = (
        conv_taps[0] * padded[:, :-2]
        + conv_taps[1] * padded[:, 1:-1]
        + conv_taps[2] * padded[:, 2:]
    )
    return convolved.reshape(product_in.shape)


def general_local(
    tokens, mix_gain, w_gate_b, w_gate_c, w_conv_in, conv_taps, w_mix_out, ffn_gain,
    w_ffn_gate, w_ffn_up, w_ffn_down,
):
    def scatter(product):
        return lax.psum_scatter(
            product.astype(BF16), "tp", scatter_dimension=0, tiled=True
        ).astype(F32)

    def dot(a, b):
        return jnp.dot(a, b, preferred_element_type=F32)

    def rows(w):
        return lax.all_gather(w, "fs", axis=0, tiled=True)

    normed = rms_scale(tokens.astype(F32), mix_gain).astype(BF16)
    gate_b, gate_c, conv_in = (dot(normed, rows(w)) for w in (w_gate_b, w_gate_c, w_conv_in))
    gated = (gate_b * causal_mix(gate_c * conv_in, conv_taps)).astype(BF16)
    row_count = normed.shape[0] // lax.axis_size("tp")
    branch = scatter(dot(gated, lax.all_gather(w_mix_out, "fs", axis=1, tiled=True)))
    own = lax.dynamic_slice_in_dim(tokens, lax.axis_index("tp") * row_count, row_count, 0)
    stream = own.astype(F32) + branch
    normed_two = lax.all_gather(
        rms_scale(stream, ffn_gain).astype(BF16), "tp", axis=0, tiled=True
    )
    hidden = (jax.nn.silu(dot(normed_two, rows(w_ffn_gate))) * dot(normed_two, rows(w_ffn_up))).astype(BF16)
    ffn_branch = scatter(dot(hidden, lax.all_gather(w_ffn_down, "fs", axis=1, tiled=True)))
    return (stream + ffn_branch).astype(BF16)


def solution(mesh):
    in_specs = (
        P(("rep", "fs"), None),
        P(),
        P("fs", "tp"),
        P("fs", "tp"),
        P("fs", "tp"),
        P(None, "tp"),
        P("tp", "fs"),
        P(),
        P("fs", "tp"),
        P("fs", "tp"),
        P("tp", "fs"),
    )
    out_specs = P(("rep", "fs", "tp"), None)
    size = mesh.shape
    square = size["tp"] == 2 and size["fs"] == 4 and size["rep"] % 2 == 0

    def local(*arrays):
        rows, width = arrays[0].shape
        channels, hidden = arrays[2].shape[1], arrays[8].shape[1]
        fits = (
            square
            and rows % (4 * LEN) == 0
            and channels % (2 * LANES) == 0
            and hidden % LANES == 0
            and hidden >= 10 * LANES
            and width % (16 * LANES) == 0
        )
        return (paired_local if fits else general_local)(*arrays)

    return jax.shard_map(local, mesh=mesh, in_specs=in_specs, out_specs=out_specs, check_vma=False)
```

```python
import jax
import jax.numpy as jnp
from jax import lax
from jax.experimental import pallas as pl
from jax.experimental.pallas import tpu as pltpu
from jax.sharding import PartitionSpec as P

LEN = 128
LANES = 128
EPSILON = 1e-06
MESH = pl.DeviceIdType.MESH
F32 = jnp.float32
BF16 = jnp.bfloat16


def rms_scale(values, gain):
    return values * lax.rsqrt(jnp.mean(values * values, axis=-1, keepdims=True) + EPSILON) * gain


N_CHUNKS = 4


def weight_pieces(rows_d, n_conv, n_mix, n_gate_up, n_down, mix_rows, down_rows):
    pieces = [(0, i * rows_d // 2, rows_d // 2, 0, n_conv) for i in range(2)]
    pieces.append((1, 0, mix_rows, 0, n_mix))
    units = n_gate_up // (2 * LANES)
    gate_up = sorted({2 * LANES * u for u in (2 * units // 5, 4 * units // 5, units)} | {0, n_gate_up})
    down = (0, n_down // 2, 3 * n_down // 4, n_down)
    for weight, rows, cuts in ((2, rows_d, gate_up), (3, down_rows, down)):
        pieces += [(weight, 0, rows, a, b - a) for a, b in zip(cuts, cuts[1:])]
    return pieces


def layer_kernel(
    tokens, wb, wc, wi, wm_in, wg_in, wu_in, wd_in, mix_gain_in, taps_in, ffn_gain_in,
    out,
    tok, normed, n2, WA, WM, WG, WD, tile, gated, MP, RS, BR, hidden, OP, RO, ZC, RF, mix_gain, taps, ffn_gain,
    load_sem, ds, dr, fs_, fr, tz_s, tz_r, ts_s, ts_r, g_s, g_r, sib_s, sib_r, z_s, z_r, n_s, n_r,
    o_s, o_r, q_s, q_r,
):
    n_fs, rows_d, _ = WA.shape
    ch = gated.shape[2]
    hid = hidden.shape[1]
    width = tokens.shape[1]
    half = tokens.shape[0] // 4
    cols = WD.shape[2]
    mcols = WM.shape[2]
    full, rest = hid // LANES, hid % LANES

    r = lax.axis_index("rep")
    f = lax.axis_index("fs")
    t = lax.axis_index("tp")
    p = lax.rem(r, 2)
    z_dev = {"rep": r + 1 - 2 * p}
    x_of = f + 1 - 2 * lax.rem(f, 2)
    y_of = lax.rem(f + 2, 4)
    d_of = lax.rem(x_of + 2, 4)
    x_dev, y_dev, s_dev = {"fs": x_of}, {"fs": y_of}, {"tp": 1 - t}

    def part(c, core):
        return pl.ds(pl.multiple_of((2 * c + core) * half, half), half)

    def chunk(c):
        return pl.ds(pl.multiple_of(2 * c * half, 2 * half), 2 * half)

    barrier = pltpu.get_barrier_semaphore()
    for dev in (x_dev, y_dev, z_dev, s_dev):
        pl.semaphore_signal(barrier, inc=1, device_id=dev, device_id_type=MESH)

    chan = pl.ds(pl.multiple_of(p * ch, ch), ch)
    loads = []

    def load(src, dst):
        c = pltpu.make_async_copy(src, dst, load_sem.at[len(loads)])
        c.start()
        loads.append(c)
        return c

    l_wa = []
    for k in range(2):
        rows = pl.ds(k * (rows_d // 2), rows_d // 2)
        l_wa.append([
            load(w.at[rows, chan], WA.at[f, rows, pl.ds(i * ch, ch)]) for i, w in enumerate((wb, wc, wi))
        ])
    l_tok = [
        load(tokens.at[pl.ds((2 * core + h) * half, half)], tok.at[part(2 * h + p, core)])
        for h in range(2) for core in range(2)
    ]
    l_small = [
        load(a, b) for a, b in ((mix_gain_in, mix_gain), (taps_in, taps), (ffn_gain_in, ffn_gain))
    ]
    pl.semaphore_wait(barrier, 4)

    def remote(src, dst, s, rcv, dev):
        return pltpu.make_async_remote_copy(
            src_ref=src, dst_ref=dst, send_sem=s, recv_sem=rcv, device_id=dev, device_id_type=MESH
        )

    bufs = (WA, WM, WG, WD)
    pieces = weight_pieces(rows_d, 3 * ch, mcols, 2 * hid, cols, WM.shape[1], hid)

    def cut(k, slot, first, parts):
        w, r0, n, c0, nc = pieces[k]
        return bufs[w].at[slot, pl.ds(r0 + first * n // 2, parts * n // 2), pl.ds(c0, nc)]

    def direct(k):
        ref = cut(k, f, 0, 2)
        return [remote(ref, ref, ds.at[k, c], dr.at[k, c], dev) for c, dev in ((0, x_dev), (1, y_dev))]

    def forward(k):
        a, b = cut(k, x_of, 0, 1), cut(k, y_of, 1, 1)
        return [
            remote(b, b, fs_.at[k, 0], fr.at[k, 0], x_dev),
            remote(a, a, fs_.at[k, 1], fr.at[k, 1], y_dev),
        ]

    sent = []

    def start(*copies):
        for c in copies:
            c.start()
            sent.append(c)
        return copies

    D, F = {}, {}

    def send(*ks):
        for k in ks:
            D[k] = start(*direct(k))

    def step(k, *more):
        for c in D[k]:
            c.wait_recv()
        F[k] = start(*forward(k))
        send(*more)

    def arrived(*ks):
        for k in ks:
            for c in F[k]:
                c.wait_recv()

    for k in range(2):
        for c in l_wa[k]:
            c.wait()
        send(k)
    for c in l_tok + l_small:
        c.wait()
    tz, ts = [], []
    for h in range(2):
        ref = tok.at[part(2 * h + p, t)]
        tz += start(remote(ref, ref, tz_s.at[h], tz_r.at[h], z_dev))

    def relay(h):
        tz[h].wait_recv()
        ref = tok.at[part(2 * h + 1 - p, t)]
        ts.extend(start(remote(ref, ref, ts_s.at[h], ts_r.at[h], s_dev)))

    def norm_chunk(c):
        def body(i, _):
            rows = pl.ds(pl.multiple_of(2 * c * half + i * 64, 64), 64)
            normed[rows, :] = rms_scale(tok[rows, :].astype(F32), mix_gain[...]).astype(BF16)
            return 0

        lax.fori_loop(0, 2 * half // 64, body, 0)

    l_rest = [load(wm_in.at[:, pl.ds(pl.multiple_of(p * mcols, mcols), mcols)], WM.at[f])]
    far = (full + (1 if rest else 0)) * LANES
    for i, w in enumerate((wg_in, wu_in)):
        for c in range(full):
            col = pl.ds(pl.multiple_of(p * far + c * LANES, LANES), LANES)
            l_rest.append(load(w.at[:, col], WG.at[f, :, pl.ds((2 * c + i) * LANES, LANES)]))
        if rest:
            l_rest.append(load(w.at[:, pl.ds(full * LANES, LANES)], tile.at[i]))
    aligned = full * LANES
    l_rest.append(load(wd_in.at[pl.ds(pl.multiple_of(p * far, LANES), aligned)], WD.at[f, pl.ds(0, aligned)]))
    if rest:
        l_rest.append(load(
            wd_in.at[pl.ds(pl.multiple_of(aligned + p * rest, rest), rest)],
            WD.at[f, pl.ds(aligned, rest)],
        ))


    norm_chunk(p)
    norm_chunk(2 + p)
    for c in l_rest:
        c.wait()
    if rest:
        gate, up = tile[0].astype(F32), tile[1].astype(F32)
        lane = lax.broadcasted_iota(jnp.int32, gate.shape, 1)
        low = jnp.where(lane < rest, gate, pltpu.roll(up, rest, 1))
        high = jnp.where(lane < rest, pltpu.roll(gate, rest, 1), up)
        WG[f, :, 2 * aligned:] = jnp.where(p == 0, low, high).astype(BF16)
    step(0, 2)
    relay(0)
    step(1)
    ts[0].wait_recv()
    norm_chunk(1 - p)
    relay(1)
    step(2, 3, 4)
    ts[1].wait_recv()
    norm_chunk(3 - p)
    arrived(0, 1)

    tap = [taps[pl.ds(i, 1), chan] for i in range(3)]
    pos = lax.rem(lax.broadcasted_iota(jnp.int32, (2 * half, ch), 0), LEN)

    def mix_in(c):
        x = normed[chunk(c), :]

        def proj(q):
            w = WA[:, :, q * ch:(q + 1) * ch].reshape(width, ch)
            return jnp.dot(x, w, preferred_element_type=F32)

        pr = proj(1) * proj(2)
        one = jnp.where(pos >= 1, pltpu.roll(pr, 1, 0), 0.0)
        two = jnp.where(pos >= 2, pltpu.roll(pr, 2, 0), 0.0)
        conv = tap[0] * two + tap[1] * one + tap[2] * pr
        gated[p, chunk(c), :] = (proj(0) * conv).astype(BF16)
        ref = gated.at[p, chunk(c)]
        gz.extend(start(remote(ref, ref, g_s.at[c], g_r.at[c], z_dev)))

    gz, sib, zc, nb = [], [], [], []

    def mix_out(c):
        gz[c].wait_recv()
        g = jnp.concatenate([gated[0, chunk(c), :], gated[1, chunk(c), :]], axis=1)
        for s in range(n_fs):
            MP[chunk(c), s * mcols:(s + 1) * mcols] = jnp.dot(
                g, WM[s], preferred_element_type=F32
            ).astype(BF16)
        sib.extend(start(remote(MP.at[part(c, 1 - t)], RS.at[c], sib_s.at[c], sib_r.at[c], s_dev)))

    def mix_pair(c):
        sib[c].wait_recv()
        BR[p, c] = (MP[part(c, t), :].astype(F32) + RS[c].astype(F32)).astype(BF16)
        zc.extend(start(remote(BR.at[p, c], BR.at[p, c], z_s.at[c], z_r.at[c], z_dev)))

    for c in range(N_CHUNKS):
        mix_in(c)
    arrived(2)
    mix_out(0)
    for c in range(1, N_CHUNKS):
        mix_out(c)
        mix_pair(c - 1)
    mix_pair(N_CHUNKS - 1)

    def stream_chunk(c):
        zc[c].wait_recv()
        step_rows = 32

        def body(i, _):
            rows = pl.ds(pl.multiple_of(i * step_rows, step_rows), step_rows)
            mine = pl.ds(pl.multiple_of((2 * c + t) * half + i * step_rows, step_rows), step_rows)
            branch = jnp.concatenate(
                [BR[q, c, rows, s * mcols:(s + 1) * mcols] for s in range(n_fs) for q in range(2)], axis=1
            )
            stream = tok[mine, :].astype(F32) + branch.astype(F32)
            n2[mine, :] = rms_scale(stream, ffn_gain[...]).astype(BF16)
            return 0

        lax.fori_loop(0, half // step_rows, body, 0)
        ref = n2.at[part(c, t)]
        nb.extend(start(remote(ref, ref, n_s.at[c], n_r.at[c], s_dev)))

    def ffn_piece(k):
        arrived(k)
        _, _, _, c0, nc = pieces[k]

        def body(i, _):
            rows = pl.ds(pl.multiple_of(4 * i * half, 4 * half), 4 * half)
            x = n2[rows, :]
            for a in range(c0, c0 + nc, 2 * LANES):
                n = min(2 * LANES, c0 + nc - a) // 2
                w = WG[:, :, a:a + 2 * n].reshape(width, 2 * n)
                zz = jnp.dot(x, w, preferred_element_type=F32)
                g, u = zz[:, :n], zz[:, n:]
                hidden[rows, a // 2:a // 2 + n] = (g / (1.0 + jnp.exp(-g)) * u).astype(BF16)
            return 0

        lax.fori_loop(0, N_CHUNKS // 2, body, 0)

    step(3, 5)
    stream_chunk(0)
    stream_chunk(1)
    step(4, 6)
    stream_chunk(2)
    stream_chunk(3)
    for c in nb:
        c.wait_recv()
    ffn_piece(3)
    step(5)
    ffn_piece(4)
    step(6, 7, 8)
    ffn_piece(5)
    ffn_piece(6)

    cuts = [pieces[k][3:] for k in (7, 8, 9)]
    blocks = [(f, 0, cols)]
    blocks += [(x_of, *cuts[0]), (y_of, *cuts[0])]
    blocks += [(x_of, *cuts[1]), (y_of, *cuts[1]), (d_of, *cuts[0])]
    blocks += [(x_of, *cuts[2]), (y_of, *cuts[2]), (d_of, *cuts[1]), (d_of, *cuts[2])]
    so, qo = [], []

    def down_send(*ks):
        for k in ks:
            s, c0, nc = blocks[k]
            cs = pl.ds(c0, nc)

            def body(i, _, s=s, c0=c0, nc=nc):
                rows = pl.ds(pl.multiple_of(4 * i * half, 4 * half), 4 * half)
                prod = jnp.dot(
                    hidden[rows, :], WD[s, :, c0:c0 + nc], preferred_element_type=F32
                ).astype(BF16)
                for e in range(4):
                    OP[s, e % 2, 2 * i + e // 2, :, c0:c0 + nc] = prod[e * half:(e + 1) * half]
                return 0

            lax.fori_loop(0, N_CHUNKS // 2, body, 0)
            so.extend(start(remote(
                OP.at[s, 1 - t, :, :, cs], RO.at[s, :, :, cs], o_s.at[k], o_r.at[k], s_dev
            )))

    def down_pair(*ks):
        for k in ks:
            so[k].wait_recv()
            s, c0, nc = blocks[k]
            cs = pl.ds(c0, nc)
            for h in range(2):
                c = 2 * h + 1 - p
                ZC[s, h, :, cs] = (OP[s, t, c, :, cs].astype(F32) + RO[s, c, :, cs].astype(F32)).astype(BF16)
            qo.extend(start(remote(
                ZC.at[s, :, :, cs], RF.at[s, :, :, cs], q_s.at[k], q_r.at[k], z_dev
            )))

    def finish(*ks):
        for k in ks:
            qo[k].wait_recv()
            s, c0, nc = blocks[k]
            for a in range(0, nc, LANES):
                lo = c0 + a
                q, at = lo // mcols, lo % mcols
                cs = pl.ds(lo, LANES)
                ms = pl.ds(pl.multiple_of(s * mcols + at, LANES), LANES)
                whole = pl.ds(pl.multiple_of(s * cols + lo, LANES), LANES)
                for h in range(2):
                    c = 2 * h + p
                    stream = tok[part(c, t), whole].astype(F32) + BR[q, c, :, ms].astype(F32)
                    branch = (
                        OP[s, t, c, :, cs].astype(F32)
                        + RO[s, c, :, cs].astype(F32)
                        + RF[s, h, :, cs].astype(F32)
                    )
                    out[h * half:(h + 1) * half, whole] = (stream + branch).astype(BF16)

    down_send(0)
    step(7, 9)
    down_pair(0)
    down_send(1, 2)
    down_pair(1, 2)
    step(8)
    down_send(3, 4)
    down_pair(3, 4)
    arrived(7)
    down_send(5)
    step(9)
    down_pair(5)
    down_send(6, 7)
    down_pair(6, 7)
    finish(0, 1, 2)
    arrived(8)
    down_send(8)
    down_pair(8)
    finish(3, 4)
    arrived(9)
    down_send(9)
    down_pair(9)
    finish(5, 6, 7, 8, 9)
    for c in sent:
        c.wait_send()


def paired_local(
    tokens, mix_gain, w_gate_b, w_gate_c, w_conv_in, conv_taps, w_mix_out, ffn_gain,
    w_ffn_gate, w_ffn_up, w_ffn_down,
):
    chip_rows, width = tokens.shape
    n_fs = lax.axis_size("fs")
    rows_d = w_gate_b.shape[0]
    ch = w_gate_b.shape[1] // 2
    hid = w_ffn_gate.shape[1] // 2
    cols = w_mix_out.shape[1]
    half = chip_rows // 4
    group = 2 * chip_rows
    n_pieces = len(weight_pieces(rows_d, 3 * ch, cols // 2, 2 * hid, cols, 2 * ch, hid))
    n_blocks = 10
    n_loads = 20 + 2 * (hid // LANES)

    def vmem(*shape):
        return pltpu.VMEM(shape, BF16)

    def dma(*shape):
        return pltpu.SemaphoreType.DMA(shape)

    return pl.pallas_call(
        layer_kernel,
        out_shape=jax.ShapeDtypeStruct((2 * half, width), BF16),
        in_specs=[pl.BlockSpec(memory_space=pl.ANY)] * 11,
        out_specs=pl.BlockSpec(memory_space=pltpu.VMEM),
        scratch_shapes=[
            vmem(group, width),
            vmem(group, width),
            vmem(group, width),
            vmem(n_fs, rows_d, 3 * ch),
            vmem(n_fs, 2 * ch, cols // 2),
            vmem(n_fs, rows_d, 2 * hid),
            vmem(n_fs, hid, cols),
            vmem(2, rows_d, LANES),
            vmem(2, group, ch),
            vmem(group, width // 2),
            vmem(N_CHUNKS, half, width // 2),
            vmem(2, N_CHUNKS, half, width // 2),
            vmem(group, hid),
            vmem(n_fs, 2, N_CHUNKS, half, cols),
            vmem(n_fs, N_CHUNKS, half, cols),
            vmem(n_fs, 2, half, cols),
            vmem(n_fs, 2, half, cols),
            pltpu.VMEM((1, width), F32),
            pltpu.VMEM(conv_taps.shape, F32),
            pltpu.VMEM((1, width), F32),
            dma(n_loads),
            *[dma(n_pieces, 2)] * 4,
            *[dma(2)] * 4,
            *[dma(N_CHUNKS)] * 8,
            *[dma(n_blocks)] * 4,
        ],
        compiler_params=pltpu.CompilerParams(
            collective_id=0, has_side_effects=True, vmem_limit_bytes=60 * 2**20
        ),
    )(
        tokens, w_gate_b, w_gate_c, w_conv_in, w_mix_out, w_ffn_gate, w_ffn_up, w_ffn_down,
        mix_gain.reshape(1, width), conv_taps, ffn_gain.reshape(1, width),
    )


def causal_mix(product_in, conv_taps):
    shaped = product_in.reshape(product_in.shape[0] // LEN, LEN, product_in.shape[1])
    padded = jnp.pad(shaped, ((0, 0), (2, 0), (0, 0)))
    convolved = (
        conv_taps[0] * padded[:, :-2]
        + conv_taps[1] * padded[:, 1:-1]
        + conv_taps[2] * padded[:, 2:]
    )
    return convolved.reshape(product_in.shape)


def general_local(
    tokens, mix_gain, w_gate_b, w_gate_c, w_conv_in, conv_taps, w_mix_out, ffn_gain,
    w_ffn_gate, w_ffn_up, w_ffn_down,
):
    def scatter(product):
        return lax.psum_scatter(
            product.astype(BF16), "tp", scatter_dimension=0, tiled=True
        ).astype(F32)

    def dot(a, b):
        return jnp.dot(a, b, preferred_element_type=F32)

    def rows(w):
        return lax.all_gather(w, "fs", axis=0, tiled=True)

    normed = rms_scale(tokens.astype(F32), mix_gain).astype(BF16)
    gate_b, gate_c, conv_in = (dot(normed, rows(w)) for w in (w_gate_b, w_gate_c, w_conv_in))
    gated = (gate_b * causal_mix(gate_c * conv_in, conv_taps)).astype(BF16)
    row_count = normed.shape[0] // lax.axis_size("tp")
    branch = scatter(dot(gated, lax.all_gather(w_mix_out, "fs", axis=1, tiled=True)))
    own = lax.dynamic_slice_in_dim(tokens, lax.axis_index("tp") * row_count, row_count, 0)
    stream = own.astype(F32) + branch
    normed_two = lax.all_gather(
        rms_scale(stream, ffn_gain).astype(BF16), "tp", axis=0, tiled=True
    )
    hidden = (jax.nn.silu(dot(normed_two, rows(w_ffn_gate))) * dot(normed_two, rows(w_ffn_up))).astype(BF16)
    ffn_branch = scatter(dot(hidden, lax.all_gather(w_ffn_down, "fs", axis=1, tiled=True)))
    return (stream + ffn_branch).astype(BF16)


def solution(mesh):
    in_specs = (
        P(("rep", "fs"), None),
        P(),
        P("fs", "tp"),
        P("fs", "tp"),
        P("fs", "tp"),
        P(None, "tp"),
        P("tp", "fs"),
        P(),
        P("fs", "tp"),
        P("fs", "tp"),
        P("tp", "fs"),
    )
    out_specs = P(("rep", "fs", "tp"), None)
    size = mesh.shape
    square = size["tp"] == 2 and size["fs"] == 4 and size["rep"] % 2 == 0

    def local(*arrays):
        rows, width = arrays[0].shape
        channels, hidden = arrays[2].shape[1], arrays[8].shape[1]
        fits = (
            square
            and rows % (4 * LEN) == 0
            and channels % (2 * LANES) == 0
            and hidden % LANES == 0
            and hidden >= 10 * LANES
            and width % (16 * LANES) == 0
        )
        return (paired_local if fits else general_local)(*arrays)

    return jax.shard_map(local, mesh=mesh, in_specs=in_specs, out_specs=out_specs, check_vma=False)
```
